32 devices in a mesh: st: 8 (over z, x), tp: 4 (over y, core).
Axes of the slice: x: 2, y: 2, z: 4, core: 2. Of those that a mesh axis runs over, the one named last changes fastest.
Arguments:
- tokens: bfloat16 [4096, 2048], P('st'), may hold values from -6 to 6
- mix_query: bfloat16 [2048, 1024], P(None, 'tp'), may hold values from -0.125 to 0.125
- mix_key: bfloat16 [2048, 1024], P(None, 'tp'), may hold values from -0.125 to 0.125
- mix_value: bfloat16 [2048, 1024], P(None, 'tp'), may hold values from -0.125 to 0.125
- decay_lower_map: bfloat16 [2048, 64], replicated, may hold values from -0.125 to 0.125
- decay_upper_map: bfloat16 [64, 1024], P(None, 'tp'), may hold values from -1 to 1
- decay_base: float32 [1024], P('tp'), may hold values from -7.5 to -2.5
- decay_shift: float32 [4096, 16], P('st', 'tp'), may hold values from -3.8 to 9.8
- rate_lower_map: bfloat16 [2048, 64], replicated, may hold values from -0.125 to 0.125
- rate_upper_map: bfloat16 [64, 1024], P(None, 'tp'), may hold values from -0.75 to 0.75
- norm_gain: float32 [1024], P('tp'), may hold values from 0.1 to 1.9
- mix_out: bfloat16 [1024, 2048], P(None, 'tp'), may hold values from -0.1875 to 0.1875
- cross_query: bfloat16 [2048, 2048], P(None, 'tp'), may hold values from -0.125 to 0.125
- score_gain: float32 [2048], P('tp'), may hold values from 0.1 to 1.9
- passage_key: bfloat16 [2048, 2048], P(None, 'tp'), may hold values from -0.125 to 0.125
- passage_value: bfloat16 [2048, 2048], P(None, 'tp'), may hold values from -0.125 to 0.125
- cross_out: bfloat16 [2048, 2048], P(None, 'tp'), may hold values from -0.5 to 0.5
- gate_down: bfloat16 [2048, 128], replicated, may hold values from -0.125 to 0.125
- gate_up: bfloat16 [128, 2048], P(None, 'tp'), may hold values from -0.5 to 0.5
- store: bfloat16 [96, 96, 2048], P('st'), may hold values from -6 to 6
- passage_ids: int32 [64, 4], P('st'), may hold values from 0 to 95, as said below
Outputs:
- mixed: bfloat16 [4096, 2048], P('st', 'tp')
The draws below stay inside these ranges and needn't reach their ends.
Inputs may be any that keep to these rules, and one draw needn't show every extreme that they name: `passage_ids`: among the 32 passages named by the rows of one sequence, at most 4 are held by one index of st (passage p by index p // 12); in every draw exactly 4 are held by the index before the sequence's own.
All inputs are finite; a program needn't handle non-finite values.
Results may differ from the reference program's by a relative error of at most 0.0075.
Values may be sent and summed in bfloat16 or wider, within the bound.
A program may use at most 128 MiB of HBM per device.

```python
import jax
import jax.numpy as jnp
from jax import lax

MODEL_DIM = 2048
MIXER_HEADS = 16
RHEAD = 64
XHEADS = 8
XHEAD = 256
LOWRANK_WIDTH = 64
GLORA = 128
PLEN = 96
PER_BLOCK = 4
QBLOCK = 64
MBLOCK = 64
TOKENS_PER_SEQ = 512
PASS_DEV = 12
MIXER_WIDTH = 1024
XWIDTH = 2048
TOKEN_TOTAL = 4096
NPASS = 96
N_ST = 8


def draw_decay_shift(key, part):
    sequence_number = TOKEN_TOTAL // TOKENS_PER_SEQ
    span_count = TOKENS_PER_SEQ // MBLOCK
    base_key, spot_key, random_size_key = jax.random.split(key, 3)
    shift_baseline = jax.random.uniform(base_key, (sequence_number, span_count, 1, 1), jnp.float32, -0.8, 0.8)
    shift_baseline = jnp.broadcast_to(shift_baseline, (sequence_number, span_count, MBLOCK, MIXER_HEADS))
    shift_baseline = shift_baseline.reshape(sequence_number, TOKENS_PER_SEQ, MIXER_HEADS)
    spot_pos = jax.random.randint(spot_key, (sequence_number, 3, MIXER_HEADS), 0, TOKENS_PER_SEQ)
    target_location = jnp.arange(TOKENS_PER_SEQ)[None, :, None, None] == spot_pos[:, None, :, :]
    spike_addition = jnp.any(target_location, axis=2).astype(jnp.float32)
    spike_addition = spike_addition * jax.random.uniform(random_size_key, (sequence_number, TOKENS_PER_SEQ, MIXER_HEADS), jnp.float32, 7.0, 9.0)
    return (shift_baseline + spike_addition).reshape(TOKEN_TOTAL, MIXER_HEADS)


def draw_passage_ids(key, part):
    blk_dev = TOKENS_PER_SEQ // QBLOCK
    slot_count = blk_dev * PER_BLOCK
    capacity = max(2, -(-slot_count // N_ST))
    positions = N_ST * capacity

    def one_sequence(seq_key, seq_index):
        keys_five = jax.random.split(seq_key, 5)
        place = jnp.arange(positions)
        offset = place // capacity
        copy_idx = place % capacity
        forced = (offset == N_ST - 1) | (offset == N_ST // 2) & (copy_idx == 0)
        score = jax.random.randint(keys_five[0], (positions,), 0, 1 << 20)
        score = jnp.where(forced, -1, score) * positions + place
        chosen = jnp.argsort(score)[:slot_count]
        owner_of = (seq_index + offset[chosen]) % N_ST
        mixing = jax.random.randint(keys_five[1], (slot_count,), 0, 1 << 20) * slot_count + jnp.arange(slot_count)
        owner_of = owner_of[jnp.argsort(mixing)]
        local_idx = jax.random.randint(keys_five[2], (slot_count,), 0, PASS_DEV)
        local_idx = jnp.minimum(local_idx, jax.random.randint(keys_five[3], (slot_count,), 0, PASS_DEV))
        local_idx = jnp.minimum(local_idx, jax.random.randint(keys_five[4], (slot_count,), 0, PASS_DEV))
        return (owner_of * PASS_DEV + local_idx).reshape(blk_dev, PER_BLOCK)
    seq_keys = jax.random.split(jax.random.fold_in(key, 11), N_ST)
    picked = jax.vmap(one_sequence)(seq_keys, jnp.arange(N_ST))
    return picked.reshape(N_ST * blk_dev, PER_BLOCK).astype(jnp.int32)


def block_levels(own_key, shape, shards, least, high):
    factor_of = 1.0
    for dim, blocks in shards:
        heights = jax.random.uniform(jax.random.fold_in(jax.random.fold_in(own_key, 6), dim), (blocks,), jnp.float32, least / len(shards), high / len(shards))
        factor_of = factor_of * jnp.repeat(jnp.exp(heights), shape[dim] // blocks).reshape((-1,) + (1,) * (len(shape) - 1 - dim))
    return factor_of


def noise(own_key, shape, width, bound, cuts=(), dtype=jnp.bfloat16):
    level = block_levels(own_key, shape, cuts, -0.22, 0.18) if cuts else 1.0
    entries = jax.random.normal(own_key, shape, jnp.float32) * width * level
    return jnp.minimum(jnp.maximum(entries, -bound), bound).astype(dtype)


def setup_inputs(seed: int = 0) -> dict:
    keys = jax.random.split(jax.random.key(seed), 22)
    tokens = noise(keys[0], (TOKEN_TOTAL, MODEL_DIM), 1.0, 6.0, ((0, 8),))
    mix_query = noise(keys[1], (MODEL_DIM, MIXER_WIDTH), MODEL_DIM ** -0.5, 0.125, ((1, 4),))
    mix_key = noise(keys[2], (MODEL_DIM, MIXER_WIDTH), MODEL_DIM ** -0.5, 0.125, ((1, 4),))
    mix_value = noise(keys[3], (MODEL_DIM, MIXER_WIDTH), MODEL_DIM ** -0.5, 0.125, ((1, 4),))
    decay_lower_map = noise(keys[4], (MODEL_DIM, LOWRANK_WIDTH), MODEL_DIM ** -0.5, 0.125)
    decay_upper_map = noise(keys[5], (LOWRANK_WIDTH, MIXER_WIDTH), (LOWRANK_WIDTH // 2) ** -0.5, 1.0, ((1, 4),))
    decay_base = jnp.clip(-7.5 + 5.0 * jax.random.uniform(keys[6], (MIXER_WIDTH,), jnp.float32) ** block_levels(keys[6], (MIXER_WIDTH,), ((0, 4),), -0.2, 0.2), -7.5, -2.5)
    decay_shift = draw_decay_shift(jax.random.fold_in(keys[21], 71), 0)
    rate_lower_map = noise(keys[8], (MODEL_DIM, LOWRANK_WIDTH), MODEL_DIM ** -0.5, 0.125)
    rate_upper_map = noise(keys[9], (LOWRANK_WIDTH, MIXER_WIDTH), LOWRANK_WIDTH ** -0.5, 0.75, ((1, 4),))
    norm_gain = jnp.clip(1.0 + 0.18 * jax.random.normal(keys[10], (MIXER_WIDTH,), jnp.float32), 0.1, 1.9)
    mix_out = noise(keys[11], (MIXER_WIDTH, MODEL_DIM), MIXER_WIDTH ** -0.5, 0.1875, ((1, 4),))
    cross_query = noise(keys[12], (MODEL_DIM, XWIDTH), MODEL_DIM ** -0.5, 0.125, ((1, 4),))
    score_gain = jnp.clip(1.0 + 0.18 * jax.random.normal(keys[13], (XWIDTH,), jnp.float32), 0.1, 1.9)
    passage_key = noise(keys[14], (MODEL_DIM, XWIDTH), MODEL_DIM ** -0.5, 0.125, ((1, 4),))
    passage_value = noise(keys[15], (MODEL_DIM, XWIDTH), MODEL_DIM ** -0.5, 0.125, ((1, 4),))
    cross_out = noise(keys[16], (XWIDTH, MODEL_DIM), (XWIDTH // 16) ** -0.5, 0.5, ((1, 4),))
    gate_down = noise(keys[17], (MODEL_DIM, GLORA), MODEL_DIM ** -0.5, 0.125)
    gate_up = noise(keys[18], (GLORA, MODEL_DIM), GLORA ** -0.5, 0.5, ((1, 4),))
    store = noise(keys[19], (NPASS, PLEN, MODEL_DIM), 1.0, 6.0, ((0, 8),))
    passage_ids = draw_passage_ids(jax.random.fold_in(keys[21], 71), 0)
    return dict(tokens=tokens, mix_query=mix_query, mix_key=mix_key, mix_value=mix_value, decay_lower_map=decay_lower_map, decay_upper_map=decay_upper_map, decay_base=decay_base, decay_shift=decay_shift, rate_lower_map=rate_lower_map, rate_upper_map=rate_upper_map, norm_gain=norm_gain, mix_out=mix_out, cross_query=cross_query, score_gain=score_gain, passage_key=passage_key, passage_value=passage_value, cross_out=cross_out, gate_down=gate_down, gate_up=gate_up, store=store, passage_ids=passage_ids)


FLOAT32 = jnp.float32
BFLOAT = jnp.bfloat16
PRECISE = lax.Precision.HIGHEST

def rounded(values):
    return lax.optimization_barrier(values.astype(BFLOAT)).astype(FLOAT32)

def head_norm(values, head_size):
    shaped = values.reshape(values.shape[:-1] + (values.shape[-1] // head_size, head_size))
    scaled = shaped * lax.rsqrt(lax.optimization_barrier(jnp.mean(shaped * shaped, axis=-1, keepdims=True)) + 1e-06)
    return scaled.reshape(values.shape)

def recurrent_step(state, inputs):
    query_vec, fade_t, key_vec, value_vec, unit_key, rate_gate = inputs
    pulled = jnp.einsum('bhij,bhj->bhi', state, -unit_key, precision=PRECISE)
    state = state * fade_t[:, :, None, :] + pulled[..., :, None] * (unit_key * rate_gate)[..., None, :] + value_vec[..., :, None] * key_vec[..., None, :]
    return (state, jnp.einsum('bhij,bhj->bhi', state, query_vec, precision=PRECISE))

def reference(tokens, mix_query, mix_key, mix_value, decay_lower_map, decay_upper_map, decay_base, decay_shift, rate_lower_map, rate_upper_map, norm_gain, mix_out, cross_query, score_gain, passage_key, passage_value, cross_out, gate_down, gate_up, store, passage_ids):
    total_rows = tokens.shape[0]
    sequence_number = total_rows // TOKENS_PER_SEQ

    def project(weight):
        return rounded(jnp.dot(tokens, weight, preferred_element_type=FLOAT32))
    query_vec = project(mix_query)
    key_vec = project(mix_key)
    value_vec = project(mix_value)
    decay_low = jnp.tanh(jnp.dot(tokens, decay_lower_map, preferred_element_type=FLOAT32)).astype(BFLOAT)
    decay_pre = decay_base + jnp.dot(decay_low, decay_upper_map, preferred_element_type=FLOAT32) + jnp.repeat(decay_shift, RHEAD, axis=1)
    log_fade = -jnp.exp(-jax.nn.softplus(-decay_pre) - 0.5)
    rate_low = jnp.dot(tokens, rate_lower_map, preferred_element_type=FLOAT32).astype(BFLOAT)
    rate_gate = jax.nn.sigmoid(jnp.dot(rate_low, rate_upper_map, preferred_element_type=FLOAT32))

    def by_time(values):
        return jnp.moveaxis(values.reshape(sequence_number, TOKENS_PER_SEQ, MIXER_HEADS, RHEAD), 1, 0)
    keyed = key_vec.reshape(total_rows, MIXER_HEADS, RHEAD)
    unit_key = keyed * lax.rsqrt(lax.optimization_barrier(jnp.sum(keyed * keyed, axis=-1, keepdims=True)) + 1e-06)
    sequence_in = (by_time(query_vec), by_time(jnp.exp(log_fade)), by_time(key_vec), by_time(value_vec), by_time(unit_key), by_time(rate_gate))
    state_zero = jnp.zeros((sequence_number, MIXER_HEADS, RHEAD, RHEAD), FLOAT32)
    _, head_out = lax.scan(recurrent_step, state_zero, sequence_in)
    head_out = jnp.moveaxis(head_out, 0, 1).reshape(total_rows, MIXER_HEADS, RHEAD)
    centred = head_out - lax.optimization_barrier(jnp.mean(head_out, axis=-1, keepdims=True))
    spread = lax.optimization_barrier(jnp.mean(centred * centred, axis=-1, keepdims=True))
    mixer_heads = (centred * lax.rsqrt(spread + 0.00064)).reshape(total_rows, MIXER_WIDTH)
    mixer_heads = (mixer_heads * norm_gain).astype(BFLOAT)
    queries = head_norm(jnp.dot(tokens, cross_query, preferred_element_type=FLOAT32), XHEAD) * score_gain
    queries = queries.astype(BFLOAT)
    store_rows = store.reshape(-1, MODEL_DIM)
    keys_all = head_norm(jnp.dot(store_rows, passage_key, preferred_element_type=FLOAT32), XHEAD)
    keys_all = keys_all.astype(BFLOAT).reshape(-1, PLEN, XWIDTH)
    values_all = jnp.dot(store_rows, passage_value, preferred_element_type=FLOAT32).astype(BFLOAT)
    values_all = values_all.reshape(-1, PLEN, XWIDTH)

    def attend(item):
        block_q, block_ids = item
        block_keys = keys_all[block_ids].reshape(-1, XHEADS, XHEAD).astype(FLOAT32)
        block_values = values_all[block_ids].reshape(-1, XHEADS, XHEAD).astype(FLOAT32)
        block_q = block_q.reshape(QBLOCK, XHEADS, XHEAD).astype(FLOAT32)
        scores = jnp.einsum('qhd,khd->hqk', block_q, block_keys, precision=PRECISE) * XHEAD ** (-0.5)
        expon = jnp.exp(scores)
        weights = rounded(expon / lax.optimization_barrier(jnp.sum(expon, axis=-1, keepdims=True)))
        result = jnp.einsum('hqk,khd->qhd', weights, block_values, precision=PRECISE)
        return result.astype(BFLOAT).reshape(QBLOCK, XWIDTH)
    attended = lax.map(attend, (queries.reshape(-1, QBLOCK, XWIDTH), passage_ids)).reshape(total_rows, XWIDTH)
    gate_low = jnp.dot(tokens, gate_down, preferred_element_type=FLOAT32).astype(BFLOAT)
    gate_open = jax.nn.sigmoid(jnp.dot(gate_low, gate_up, preferred_element_type=FLOAT32))
    mixer_part = jnp.dot(mixer_heads, mix_out, preferred_element_type=FLOAT32)
    cross_part = jnp.dot(attended, cross_out, preferred_element_type=FLOAT32)
    return (mixer_part + gate_open * cross_part).astype(BFLOAT)
```

```python
import contextlib
import functools

import jax
import jax.numpy as jnp
from jax import lax
from jax.experimental import pallas as pl
from jax.experimental.pallas import tpu as pltpu
from jax.sharding import PartitionSpec as P

XHEAD = 256
QBLOCK = 64
MBLOCK = 64

FLOAT32 = jnp.float32
BFLOAT = jnp.bfloat16
MESH = pl.DeviceIdType.MESH
scope = contextlib.nullcontext
ST, TP = "st", "tp"


def split(values):
    high = values.astype(BFLOAT)
    return high, (values - high.astype(FLOAT32)).astype(BFLOAT)


def raw_dot(left, right, dims=((1,), (0,))):
    return lax.dot_general(left, right, (dims, ((), ())), preferred_element_type=FLOAT32)


def fine_dot(left, right, dims=((1,), (0,))):
    left = left[0] if isinstance(left, tuple) else left.astype(BFLOAT)
    right = right[0] if isinstance(right, tuple) else right.astype(BFLOAT)
    return raw_dot(left, right, dims)


def exact_dot(values, ones):
    return raw_dot(values.astype(BFLOAT), ones)


def iota(shape, dim):
    return lax.broadcasted_iota(jnp.int32, shape, dim)


def each(fn, *lists):
    return [fn(*items) for items in zip(*lists)]


def recur_step(heads, blocks, base, refs, gain, state_ref, out_ref):
    query_ref, key_ref, value_ref, fade_ref, gate_ref = refs
    width = query_ref.shape[1]
    size = width // heads
    rows = heads * MBLOCK
    row_head = (iota((rows, width), 0) // MBLOCK) == (iota((rows, width), 1) // size)
    state_head = (iota((width, width), 0) // size) == (iota((width, width), 1) // size)
    ones_head = jnp.where(state_head, 1.0, 0.0).astype(BFLOAT)
    row_pos = iota((rows, rows), 0) % MBLOCK
    col_pos = iota((rows, rows), 1) % MBLOCK
    strict = col_pos < row_pos
    upto = col_pos <= row_pos
    lower = jnp.where(
        iota((MBLOCK, MBLOCK), 1) <= iota((MBLOCK, MBLOCK), 0), 1.0, 0.0
    ).astype(BFLOAT)

    def expand(values):
        return jnp.where(row_head, jnp.concatenate([values] * heads, axis=0), 0.0)

    def compact(values):
        return jnp.concatenate(
            [values[:, head * size : (head + 1) * size] for head in range(heads)], axis=0
        )

    def natural(values):
        return jnp.concatenate(
            [values[head * MBLOCK : (head + 1) * MBLOCK] for head in range(heads)], axis=1
        )

    def span(block):
        return pl.ds(pl.multiple_of(base + block * MBLOCK, MBLOCK), MBLOCK)

    def load(ref):
        return [ref[span(b), :].astype(FLOAT32) for b in range(blocks)]

    def running_sum(fade):
        high, low = split(fade)
        rest = (fade - high.astype(FLOAT32) - low.astype(FLOAT32)).astype(BFLOAT)
        return raw_dot(lower, high) + (raw_dot(lower, low) + raw_dot(lower, rest))

    query, key, value = load(query_ref), load(key_ref), load(value_ref)
    fade, gate = load(fade_ref), load(gate_ref)
    cumul = each(running_sum, fade)
    unit = each(lambda k: k * lax.rsqrt(exact_dot(k * k, ones_head) + 1e-06), key)
    rate = each(lambda u, g: u * g, unit, gate)
    minus_scaled = each(lambda u, c, f: -u * jnp.exp(c - f), unit, cumul, fade)
    query_scaled = each(lambda q, c: q * jnp.exp(c), query, cumul)
    inverse = each(lambda c: jnp.exp(-c), cumul)
    fade_out = each(lambda c: jnp.exp(c[MBLOCK - 1 :, :] - c), cumul)
    block_fade = each(lambda c: jnp.exp(c[MBLOCK - 1 :, :]), cumul)
    left = each(
        lambda m, q: split(jnp.concatenate([expand(m), expand(q)], axis=0)),
        minus_scaled,
        query_scaled,
    )
    right = each(
        lambda k, r, i: split(jnp.concatenate([expand(k * i), expand(r * i)], axis=0)),
        key,
        rate,
        inverse,
    )
    pairs = each(lambda a, b: fine_dot(a, b, ((1,), (1,))), left, right)
    key_mats = each(
        lambda p: jnp.concatenate(
            [jnp.where(strict, p[:rows, :rows], 0.0), jnp.where(upto, p[rows:, :rows], 0.0)], axis=0
        ),
        pairs,
    )
    rate_pull = each(lambda p: split(jnp.where(strict, p[:rows, rows:], 0.0)), pairs)
    rate_read = each(lambda p: split(jnp.where(upto, p[rows:, rows:], 0.0)), pairs)
    value_rows = each(lambda v: compact(v).astype(BFLOAT), value)

    def key_values(mats, vals):
        return raw_dot(mats.astype(BFLOAT), vals)

    from_values = each(key_values, key_mats, value_rows)
    solved = each(
        lambda m, kv: jnp.concatenate([compact(m), kv[:rows]], axis=1), minus_scaled, from_values
    )
    power = rate_pull
    levels = (MBLOCK - 1).bit_length()
    for level in range(levels):
        solved = each(lambda s, p: s + fine_dot(p, s), solved, power)
        if level < levels - 1:
            power = each(lambda p: split(fine_dot(p, p)), power)
    solved_halves = each(split, solved)
    reads = each(
        lambda q, kv, r, s: jnp.concatenate([compact(q), kv[rows:]], axis=1) + fine_dot(r, s),
        query_scaled,
        from_values,
        rate_read,
        solved_halves,
    )
    moved = each(
        lambda s, r, f: fine_dot(s, expand(r * f), ((0,), (0,))), solved_halves, rate, fade_out
    )

    def key_update(vals, k, f):
        return raw_dot(vals, expand(k * f).astype(BFLOAT), ((0,), (0,)))

    added = each(key_update, value_rows, key, fade_out)
    carry = each(
        lambda m: split(jnp.where(state_head, jnp.concatenate([m[:size]] * heads, axis=0), 0.0)),
        moved,
    )
    added = each(lambda a, m: a + m[size:], added, moved)
    read_state = each(lambda r: split(natural(r[:, :size])), reads)
    read_fixed = each(lambda r: natural(r[:, size:]), reads)
    state = state_ref[...]
    head_out = []
    for block in range(blocks):
        spread_state = jnp.where(state_head, jnp.concatenate([state] * heads, axis=0), 0.0)
        head_out.append(
            read_fixed[block] + fine_dot(read_state[block], spread_state, ((1,), (1,)))
        )
        state = state * block_fade[block] + fine_dot(state, carry[block]) + added[block]
    state_ref[...] = state
    for block in range(blocks):
        mean = exact_dot(head_out[block], ones_head) * (1.0 / size)
        centred = head_out[block] - mean
        variance = exact_dot(centred * centred, ones_head) * (1.0 / size)
        normed = centred * lax.rsqrt(variance + 0.00064) * gain
        out_ref[0, span(block), :] = normed.astype(BFLOAT)


class Names(dict):
    __getattr__ = dict.__getitem__


def remote(src, dst, send, recv, **peer):
    return pltpu.make_async_remote_copy(
        src_ref=src,
        dst_ref=dst,
        send_sem=send,
        recv_sem=recv,
        device_id=peer,
        device_id_type=MESH,
    )


def when(valid, action):
    if valid is True:
        action()
    else:
        pl.when(valid)(action)


def layer_kernel(size, tree, *refs):
    ids, given, big, out, keep = jax.tree.unflatten(tree, refs)
    keep = Names(keep)
    small = Names(keep.small)
    n, tp, depth, wide = size.owners, size.tp, size.depth, size.wide
    lines = tp // 2
    cap, heads, per_block = size.capacity, size.cross_heads, size.per_block
    me = lax.axis_index(ST)
    mine = lax.axis_index(TP)
    level, column = me // wide, me % wide
    half = depth // 2
    upper = level // half
    base = upper * half
    hub = half - 1 + upper
    off_hub = upper * (level - hub) + (1 - upper) * (hub - level)
    hubbed = range(0)

    def seating(head):
        if head in hubbed:
            return base * wide, half * wide
        return 0, n

    line, core = mine // 2, mine % 2
    sibling = line * 2 + 1 - core

    loads = [
        pltpu.make_async_copy(src, dst, keep.load_sem.at[i])
        for i, (src, dst) in enumerate(zip(big, keep.big))
    ]
    (
        load_tokens,
        load_query,
        load_store,
        load_key,
        load_value,
        load_mix_query,
        load_mix_key,
        load_mix_value,
        load_decay,
        load_rate,
        load_gate,
        load_mix_out,
        load_cross,
    ) = loads
    (
        tokens,
        cross_query,
        store,
        passage_key,
        passage_value,
        mix_query,
        mix_key,
        mix_value,
        decay_lower,
        rate_lower,
        gate_down,
        mix_out,
        cross_out,
    ) = keep.big
    little = {
        name: pltpu.make_async_copy(given[name], small[name], keep.small_sem.at[i])
        for i, name in enumerate(given)
    }
    load_tokens.start()
    load_query.start()
    for copy in little.values():
        copy.start()

    barrier = pltpu.get_barrier_semaphore()

    @pl.loop(1, n)
    def _(d):
        pl.semaphore_signal(barrier, inc=1, device_id={ST: (me + d) % n}, device_id_type=MESH)

    for k in range(1, lines):
        peer = ((line + k) % lines) * 2 + core
        pl.semaphore_signal(barrier, inc=1, device_id={TP: peer}, device_id_type=MESH)
    pl.semaphore_signal(barrier, inc=1, device_id={TP: sibling}, device_id_type=MESH)

    slots = size.blocks * per_block
    down_slot = iota((slots, 128), 0)
    lane = iota((slots, 128), 1)
    by_lane = jnp.zeros((slots, 128), jnp.int32)
    by_slot = jnp.zeros((slots, 128), jnp.int32)
    for j in range(slots):
        ident = ids[j % per_block, j // per_block]
        by_lane = jnp.where(lane == j, ident, by_lane)
        by_slot = jnp.where(down_slot == j, ident, by_slot)
    owner_lane, owner_slot = by_lane // size.pass_dev, by_slot // size.pass_dev
    same = owner_lane == owner_slot
    valid = lane < slots

    def count(flags, axis):
        total = jnp.sum(jnp.where(flags & valid, 1, 0), axis=axis, keepdims=True)
        return jnp.minimum(total, cap - 1)

    rank_lane = count(same & (down_slot > lane), 0)
    rank_slot = count(same & (lane > down_slot), 1)
    power = jnp.ones((slots, 1), jnp.int32)
    for s in range(1, cap):
        power = jnp.where(rank_slot == s, 64**s, power)
    mine_too = owner_slot == lane - 64
    code = jnp.sum(jnp.where(mine_too, (down_slot + 1) * power, 0), axis=0, keepdims=True)
    table = jnp.where(lane[:1] < 64, by_lane[:1] * 8 + rank_lane, code)
    keep.names_out[...] = table
    keep.names_in[me] = table

    def name_copy(d):
        return remote(
            keep.names_out,
            keep.names_in.at[me],
            keep.name_send,
            keep.name_recv,
            st=(me + d) % n,
        )

    own_names = pltpu.make_async_copy(keep.names_out, keep.own, keep.own_sem)
    own_names.start()

    above = [(k, level - k >= 0, level - k) for k in range(1, depth)]
    below = [(depth - 1 + k, level + k < depth, level + k) for k in range(1, depth)]
    origins = [(0, True, level)] + above + below

    def dense_copy(head, rel, dst, target):
        return remote(
            keep.dense[head][rel],
            keep.dense[head][dst],
            keep.dense_send[head].at[dst],
            keep.dense_recv[head].at[dst],
            st=target,
        )

    def forwards(head, rel):
        moves = []
        if rel < depth - 1:
            copy = dense_copy(head, rel, rel + 1, (me + wide) % n)
            held = level < depth - 1
            moves.append(((level - rel >= 0) & held if rel else held, copy))
        if rel == 0 or depth - 1 < rel < 2 * depth - 2:
            far = rel - depth + 1 if rel else 0
            copy = dense_copy(head, rel, depth + far, (me + n - wide) % n)
            held = level > 0
            moves.append(((level + far < depth) & held if rel else held, copy))
        return moves

    def side_copy(head, rel, turn):
        slot = rel * wide + turn
        return remote(
            keep.side_out[head].at[slot],
            keep.side_in[head].at[slot],
            keep.side_send[head].at[rel * (wide - 1) + turn - 1],
            keep.side_recv[head].at[rel * (wide - 1) + turn - 1],
            st=level * wide + (column + turn) % wide,
        )

    def digit(code, s):
        return jnp.clip((code // 64**s) % 64 - 1, 0, slots - 1)

    def spread_queries(head, rel, row, where):
        for _, copy in forwards(head, rel):
            pl.when(_)(copy.start)
        for turn in range(1, wide):
            target = where * 0 + level * wide + (column + turn) % wide
            code = row(64 + target)
            for s in range(cap):
                keep.side_out[head][rel * wide + turn, s] = keep.dense[head][rel][
                    digit(code, s) // per_block
                ]
            side_copy(head, rel, turn).start()

    def from_served(source):
        return lambda index: keep.served[source, 0, index]

    for copy in little.values():
        copy.wait()
    load_tokens.wait()
    load_query.wait()
    for copy in loads[2:]:
        copy.start()

    for head in range(heads):
        with scope("q"):
            cols = pl.ds(head * XHEAD, XHEAD)
            dots = raw_dot(tokens[...], cross_query[:, cols])
            mean = jnp.mean(dots * dots, axis=-1, keepdims=True)
            queries = (dots * lax.rsqrt(mean + 1e-06) * small.score_gain[:, cols]).astype(BFLOAT)
            keep.dense[head][0][...] = queries.reshape(keep.dense[head][0].shape)
            if head == 0:
                own_names.wait()
                pl.semaphore_wait(barrier, n - 1 + lines)

                @pl.loop(1, n)
                def _(d):
                    name_copy(d).start()

            if head == 0 or not 0:
                spread_queries(head, 0, lambda index: keep.own[0, index], level)

    with scope("kv"):
        load_store.wait()
        load_key.wait()
        load_value.wait()
        length = size.passage_len
        group = 4 if size.pass_dev % 4 == 0 else 1
        chunk = group * length
        for head in range(heads):
            cols = pl.ds(head * XHEAD, XHEAD)

            @pl.loop(0, size.pass_dev // group)
            def _(i):
                rows = pl.ds(pl.multiple_of(i * chunk, chunk), chunk)
                part = pl.ds(i * group, group)
                shape = (group, length, XHEAD)
                dots = raw_dot(store[rows, :], passage_key[:, cols])
                mean = jnp.mean(dots * dots, axis=-1, keepdims=True)
                kept = (dots * lax.rsqrt(mean + 1e-06)).astype(BFLOAT)
                keep.kept_keys[head][part] = kept.reshape(shape)
                dots = raw_dot(store[rows, :], passage_value[:, cols])
                keep.kept_values[head][part] = dots.astype(BFLOAT).reshape(shape)

    with scope("names"):

        rest = keep.names_in.at[pl.ds(0, n - 1)]
        remote(rest, rest, keep.name_send, keep.name_recv, st=me).wait_recv()
        served = pltpu.make_async_copy(keep.names_in, keep.served, keep.served_sem)
        served.start()
        served.wait()

    ones = jnp.ones((8, length), BFLOAT)

    def result_copies(head, source, target, parts, sums, marks):
        seat = me - seating(head)[0]
        span = pl.ds(seat * cap, cap)
        recv, recv_sums = marks
        return (
            remote(
                keep.parts_out[head].at[source],
                parts.at[span],
                keep.part_send[head],
                recv,
                st=target,
            ),
            remote(
                keep.sums_out[head].at[source],
                sums.at[span],
                keep.sum_send[head],
                recv_sums,
                st=target,
            ),
        )

    def send_direct(head, source):
        marks = keep.part_recv[head], keep.sum_recv[head]
        for copy in result_copies(head, source, source, keep.parts[head], keep.sums[head], marks):
            copy.start()

    def send_to_hub(head, source, far):
        target = hub * wide + source % wide
        parts, sums = keep.hub_parts[head][far - 1], keep.hub_sums[head][far - 1]
        marks = keep.hub_recv[head][far - 1], keep.hub_sum_recv[head][far - 1]
        for copy in result_copies(head, source, target, parts, sums, marks):
            copy.start()

    def keep_at_hub(head, source, far):
        span = pl.ds((me - seating(head)[0]) * cap, cap)
        keep.hub_parts[head][far - 1][span] = keep.parts_out[head][source]
        keep.hub_sums[head][far - 1][span] = keep.sums_out[head][source]

    def attend(head, rel, turn, floor):
        source = floor * wide + (column + wide - turn) % wide
        local = rel == 0 and turn == 0
        row = from_served(source)
        code = row(64 + me)
        for s in range(cap):
            slot = digit(code, s)
            passage = lax.div(row(slot), 8) % size.pass_dev
            kept, vals = keep.kept_keys[head][passage], keep.kept_values[head][passage]
            if turn:
                asked = keep.side_in[head][rel * wide + turn, s]
            else:
                asked = keep.dense[head][rel][slot // per_block]
            scores = raw_dot(asked, kept, ((1,), (1,)))
            expon = jnp.exp(scores * XHEAD ** (-0.5)).astype(BFLOAT)
            result = raw_dot(expon, vals).astype(BFLOAT)
            total = raw_dot(ones, expon, ((1,), (1,)))[:1]
            total = jnp.concatenate([total, jnp.zeros_like(total)], axis=1)
            if local:
                seat = me - seating(head)[0]
                keep.parts[head][seat * cap + s] = result
                keep.sums[head][seat * cap + s] = total
            else:
                keep.parts_out[head][source, s] = result
                keep.sums_out[head][source, s] = total
        if not local and (rel == 0 or head not in hubbed):
            send_direct(head, source)
        elif rel:
            k = rel if rel < depth else rel - depth + 1
            away = floor // half != upper
            if k < half:
                pl.when(jnp.logical_not(away))(functools.partial(send_direct, head, source))
            for step in range(half):
                far = k - step
                if 1 <= far <= half:
                    send = send_to_hub if step or turn else keep_at_hub
                    pl.when(away & (off_hub == step))(functools.partial(send, head, source, far))

    def pass_on(head, k):
        for rel, valid, floor in (origins[k], origins[depth - 1 + k]):

            def arrive(rel=rel, floor=floor):
                dense_copy(head, rel, rel, me).wait_recv()
                spread_queries(head, rel, from_served(floor * wide + column), floor)

            pl.when(valid)(arrive)

    def from_side(head, k, among):
        for rel, valid, floor in (origins[k], origins[depth - 1 + k]) if k else origins[:1]:

            def arrive(rel=rel, floor=floor):
                attend(head, rel, 0, floor)
                for turn in range(1, wide):
                    side_copy(head, rel, turn).wait_recv()
                    attend(head, rel, turn, floor)

            pl.when(among if valid is True else valid & among)(arrive)

    def mixer_inputs():
        for copy in loads[5:10]:
            copy.wait()
        for weight, target in (
            (mix_query, keep.m_query),
            (mix_key, keep.m_key),
            (mix_value, keep.m_value),
        ):
            target[...] = raw_dot(tokens[...], weight[...]).astype(BFLOAT)
        low = jnp.tanh(raw_dot(tokens[...], decay_lower[...], ((1,), (1,)))).astype(BFLOAT)
        pre = small.decay_base[...] + raw_dot(low, small.decay_upper_map[...])
        lanes = iota((size.mix_heads, pre.shape[1]), 1) // (pre.shape[1] // size.mix_heads)
        chosen = iota(lanes.shape, 0) == lanes
        chosen = jnp.where(chosen, 1.0, 0.0).astype(BFLOAT)
        shift = small.decay_shift[...]
        high, middle = split(shift)
        rest = (shift - high.astype(FLOAT32) - middle.astype(FLOAT32)).astype(BFLOAT)
        first = ((0,), (0,))
        pre = pre + (
            raw_dot(high, chosen, first)
            + (raw_dot(middle, chosen, first) + raw_dot(rest, chosen, first))
        )
        keep.m_fade[...] = jax.nn.sigmoid(pre) * (-(2.718281828459045**-0.5))
        low = raw_dot(tokens[...], rate_lower[...], ((1,), (1,))).astype(BFLOAT)
        keep.m_gate[...] = jax.nn.sigmoid(raw_dot(low, small.rate_upper_map[...]))

    blocks = 2 if size.tokens % (2 * MBLOCK) == 0 else 1
    steps = size.tokens // (blocks * MBLOCK)

    def recur(first, last):
        @pl.loop(first, last)
        def _(i):
            recur_step(
                size.mix_heads,
                blocks,
                i * (blocks * MBLOCK),
                (keep.m_query, keep.m_key, keep.m_value, keep.m_fade, keep.m_gate),
                small.norm_gain[...],
                keep.state,
                keep.mixed,
            )

    def tp_copy(buf, send, recv, slot_from, slot_to, peer):
        return remote(
            buf.at[slot_from], buf.at[slot_to], send.at[slot_to], recv.at[slot_to], tp=peer
        )

    def tp_first(buf, send, recv):
        copies = [tp_copy(buf, send, recv, 0, 1, sibling)]
        for k in range(1, lines):
            peer = ((line + k) % lines) * 2 + core
            copies.append(tp_copy(buf, send, recv, 0, 2 * k, peer))
        return copies

    def tp_second(buf, send, recv):
        return [tp_copy(buf, send, recv, 2 * k, 2 * k + 1, sibling) for k in range(1, lines)]

    def origin(slot):
        k, flip = slot // 2, slot % 2
        return ((line + lines - k) % lines) * 2 + (1 - core if flip else core)

    def relay(first, second):
        for copy, forward in zip(first[1:], second):
            copy.wait_recv()
            forward.start()

    def products(buf, weights, stride, offset, acc, fresh):
        width = buf.shape[2]
        total = None if fresh else acc[...]
        for slot in range(tp):
            start = pl.multiple_of(origin(slot) * stride + offset, 128)
            term = raw_dot(buf[slot], weights[pl.ds(start, width), :])
            total = term if total is None else total + term
        acc[...] = total

    def gates():
        load_gate.wait()
        low = raw_dot(tokens[...], gate_down[...]).astype(BFLOAT)
        keep.opened[...] = jax.nn.sigmoid(raw_dot(low, small.gate_up[...]))

    diagonal = iota((QBLOCK, QBLOCK), 0) == iota((QBLOCK, QBLOCK), 1)

    def await_crowd(head, parts, sums, marks):
        low, crowd = seating(head)
        for full, sem in zip((parts, sums), marks):
            rest = full.at[pl.ds(0, (crowd - 1) * cap)]
            remote(rest, rest, sem, sem, st=me).wait_recv()

    def gather(head, entry_of, parts, sums, b):
        low, crowd = seating(head)
        total = jnp.zeros((QBLOCK, XHEAD), FLOAT32)
        row = jnp.zeros((1, 128), FLOAT32)
        for p in range(per_block):
            entry = entry_of(b * per_block + p)
            owner = lax.div(lax.div(entry, 8), size.pass_dev) - low
            inside = (owner >= 0) & (owner < crowd)
            index = jnp.where(inside, owner * cap + lax.rem(entry, 8), crowd * cap)
            total = total + parts[index].astype(FLOAT32)
            row = row + sums[index]
        return total, row

    def hub_copies(head, far):
        target = (hub + far - 2 * far * upper) * wide + column
        return (
            remote(
                keep.hub_out[head][far - 1],
                keep.far_parts[head],
                keep.hub_send[head].at[far - 1],
                keep.far_recv[head].at[0],
                st=target,
            ),
            remote(
                keep.hub_sums_out[head][far - 1],
                keep.far_sums[head],
                keep.hub_sum_send[head].at[far - 1],
                keep.far_recv[head].at[1],
                st=target,
            ),
        )

    def serve_hub(head, far):
        parts, sums = keep.hub_parts[head][far - 1], keep.hub_sums[head][far - 1]
        source = (hub + far - 2 * far * upper) * wide + column

        @pl.when(level == hub)
        def _():
            marks = keep.hub_recv[head][far - 1], keep.hub_sum_recv[head][far - 1]
            await_crowd(head, parts, sums, marks)

            @pl.loop(0, size.blocks)
            def _(b):
                total, row = gather(head, from_served(source), parts, sums, b)
                keep.hub_out[head][far - 1][b] = total.astype(BFLOAT)
                keep.hub_sums_out[head][far - 1][b] = row

            for copy in hub_copies(head, far):
                copy.start()

    def combine(head):
        parts, sums = keep.parts[head], keep.sums[head]
        buf = keep.attended[head]
        with scope("wait"):
            await_crowd(head, parts, sums, (keep.part_recv[head], keep.sum_recv[head]))
            if head in hubbed:
                for copy in hub_copies(head, 1):
                    copy.wait_recv()
        with scope("comb"):

            @pl.loop(0, size.blocks)
            def _(b):
                total, row = gather(head, lambda index: keep.own[0, index], parts, sums, b)
                if head in hubbed:
                    total = total + keep.far_parts[head][b].astype(FLOAT32)
                    row = row + keep.far_sums[head][b]
                inverse = 1.0 / row[:, :QBLOCK]
                column = jnp.sum(jnp.where(diagonal, inverse, 0.0), axis=1, keepdims=True)
                rows = pl.ds(pl.multiple_of(b * QBLOCK, QBLOCK), QBLOCK)
                buf[0, rows, :] = (total * column).astype(BFLOAT)

    every = []

    def tp_start(buf, send, recv):
        first, second = tp_first(buf, send, recv), tp_second(buf, send, recv)
        for copy in first:
            copy.start()
        every.append(first + second)
        return first, second

    def tp_finish(first, second):
        first[0].wait_recv()
        for copy in second:
            copy.wait_recv()

    def tp_attended(head):
        return tp_start(keep.attended[head], keep.att_send[head], keep.att_recv[head])

    keep.state[...] = jnp.zeros_like(keep.state)
    for head in hubbed:
        none = pl.ds(half * wide * cap, 1)
        for parts in (keep.parts[head], *keep.hub_parts[head]):
            parts[none] = jnp.zeros((1, QBLOCK, XHEAD), BFLOAT)
        for sums in (keep.sums[head], *keep.hub_sums[head]):
            sums[none] = jnp.zeros((1, 1, 128), FLOAT32)
    last = heads - 1
    hubs = []

    moves = [(k, head) for k in range(1, depth) for head in range(heads)]
    moves.sort(key=lambda move: move[0] + 0.5 * move[1])
    edge = (level == 0) | (level == depth - 1)
    queues = [
        (edge, [(head, 0) for head in range(heads)], [1,2,2,2,2,0]),
        (jnp.logical_not(edge), [(head, 0) for head in range(heads)], [9,9,9,2,0]),
    ]

    done = 0

    def catch_up(lag=None):
        with scope("side"):
            for among, waiting, lags in queues:
                keep_back = lags[0] if lag is None else lag
                if len(lags) > 1:
                    lags.pop(0)
                if len(waiting) > keep_back:
                    waiting.sort()
                while len(waiting) > keep_back:
                    from_side(*waiting.pop(0), among)

    for k, head in moves:
        if (k, head) not in moves[:2] and done < steps:
            with scope("rec"):
                recur(done, done + 1)
            done += 1
        if (k, head) == moves[-1]:
            if done < steps:
                with scope("rec"):
                    recur(done, steps)
            with scope("mixx"):
                mixer_moves = tp_start(keep.mixed, keep.mix_send, keep.mix_recv)
                gates()
        with scope("pass"):
            pass_on(head, k)
        for _, waiting, _ in queues:
            waiting.append((head, k))
        if k >= half and head in hubbed:
            hubs.append((head, k - half + 1))
        catch_up()
        if (k, head) == moves[0]:
            for other in range(1, heads if 0 else 1):
                spread_queries(other, 0, lambda index: keep.own[0, index], level)
            with scope("mixin"):
                mixer_inputs()
    catch_up(0)
    with scope("relay"):
        relay(*mixer_moves)
    with scope("hub"):
        for job in hubs:
            serve_hub(*job)
    pending = []
    for head in range(last):
        combine(head)
        pending.append(tp_attended(head))
    with scope("mix"):
        load_mix_out.wait()
        load_cross.wait()
        tp_finish(*mixer_moves)
        products(keep.mixed, mix_out, keep.mixed.shape[2], 0, keep.mix_acc, True)
    combine(last)
    pending.append(tp_attended(last))
    with scope("relay"):
        for copies in pending[:last]:
            relay(*copies)
    def settle():
        rest = keep.names_in.at[pl.ds(0, n - 1)]
        remote(rest, rest, keep.name_send, keep.name_recv, st=me).wait_send()
        for head in range(heads):
            for full, sem in ((keep.parts_out, keep.part_send), (keep.sums_out, keep.sum_send)):
                rest = full[head].at[pl.ds(0, n - 1)]
                remote(rest, rest, sem[head], sem[head], st=me).wait_send()

        @pl.when(level == hub)
        def _():
            for head in hubbed:
                for far in range(1, half + 1):
                    for copy in hub_copies(head, far):
                        copy.wait_send()

        for head in range(heads):
            for rel, valid, floor in origins:
                for held, copy in forwards(head, rel):
                    pl.when(held)(copy.wait_send)
                for turn in range(1, wide):
                    when(valid, side_copy(head, rel, turn).wait_send)

    for head in range(heads):
        if head == last:
            with scope("settle"):
                settle()
        with scope("tpx"):
            if head == last:
                relay(*pending[head])
            tp_finish(*pending[head])
        with scope("cross"):
            buf = keep.attended[head]
            products(buf, cross_out, heads * XHEAD, head * XHEAD, keep.cross_acc, head == 0)

    with scope("out"):
        out[...] = (keep.mix_acc[...] + keep.opened[...] * keep.cross_acc[...]).astype(BFLOAT)

    for copies in every:
        for copy in copies:
            copy.wait_send()


def layer(
    tokens,
    mix_query,
    mix_key,
    mix_value,
    decay_lower_map,
    decay_upper_map,
    decay_base,
    decay_shift,
    rate_lower_map,
    rate_upper_map,
    norm_gain,
    mix_out,
    cross_query,
    score_gain,
    passage_key,
    passage_value,
    cross_out,
    gate_down,
    gate_up,
    store,
    passage_ids,
):
    n, tp = lax.axis_size(ST), lax.axis_size(TP)
    rows, model = tokens.shape
    blocks, per_block = passage_ids.shape
    wide = 1
    while n % (2 * wide) == 0 and (2 * wide) ** 2 <= n:
        wide = 2 * wide
    depth = n // wide
    heads = cross_query.shape[1] // XHEAD
    size = Names(
        owners=n,
        tp=tp,
        wide=wide,
        depth=depth,
        tokens=rows,
        blocks=blocks,
        per_block=per_block,
        pass_dev=store.shape[0],
        passage_len=store.shape[1],
        capacity=max(2, -(-(blocks * per_block) // n)),
        cross_heads=heads,
        mix_heads=decay_shift.shape[1],
    )
    cap = size.capacity
    mix_width = mix_query.shape[1]
    out_cols = mix_out.shape[1]
    relatives = 2 * depth - 1
    small = dict(
        decay_upper_map=decay_upper_map,
        decay_base=decay_base.reshape(1, -1),
        decay_shift=decay_shift.T,
        rate_upper_map=rate_upper_map,
        norm_gain=norm_gain.reshape(1, -1),
        score_gain=score_gain.reshape(1, -1),
        gate_up=gate_up,
    )
    big = (
        tokens,
        cross_query,
        store.reshape(-1, model),
        passage_key,
        passage_value,
        mix_query,
        mix_key,
        mix_value,
        decay_lower_map.T,
        rate_lower_map.T,
        gate_down,
        mix_out,
        cross_out,
    )
    dma = pltpu.SemaphoreType.DMA

    def per_head(make, *shape):
        return [make(*shape) for _ in range(heads)]

    def sems(count):
        return [dma((count,)) for _ in range(heads)]

    def per_far(make, *shape):
        return [[make(*shape) for _ in range(half)] for _ in range(0)]

    query_block = (QBLOCK, XHEAD)
    half = depth // 2
    crowd = half * wide
    crowds = [n] * heads
    scratch = dict(
        big=tuple(pltpu.VMEM(array.shape, array.dtype) for array in big),
        load_sem=dma((len(big),)),
        small={name: pltpu.VMEM(array.shape, array.dtype) for name, array in small.items()},
        small_sem=dma((len(small),)),
        own=pltpu.SMEM((1, 128), jnp.int32),
        own_sem=dma,
        served=pltpu.SMEM((n, 1, 128), jnp.int32),
        served_sem=dma,
        names_out=pltpu.VMEM((1, 128), jnp.int32),
        names_in=pltpu.VMEM((n, 1, 128), jnp.int32),
        name_send=dma,
        name_recv=dma,
        dense=[
            [pltpu.VMEM((blocks,) + query_block, BFLOAT) for _ in range(relatives)]
            for _ in range(heads)
        ],
        dense_send=sems(relatives),
        dense_recv=sems(relatives),
        side_out=per_head(pltpu.VMEM, (relatives * wide, cap) + query_block, BFLOAT),
        side_in=per_head(pltpu.VMEM, (relatives * wide, cap) + query_block, BFLOAT),
        side_send=sems(relatives * (wide - 1)),
        side_recv=sems(relatives * (wide - 1)),
        parts_out=per_head(pltpu.VMEM, (n, cap) + query_block, BFLOAT),
        parts=[pltpu.VMEM((c * cap + 1,) + query_block, BFLOAT) for c in crowds],
        part_send=[dma] * heads,
        part_recv=[dma] * heads,
        sums_out=per_head(pltpu.VMEM, (n, cap, 1, 128), FLOAT32),
        sums=[pltpu.VMEM((c * cap + 1, 1, 128), FLOAT32) for c in crowds],
        sum_send=[dma] * heads,
        sum_recv=[dma] * heads,
        hub_parts=per_far(pltpu.VMEM, (crowd * cap + 1,) + query_block, BFLOAT),
        hub_sums=per_far(pltpu.VMEM, (crowd * cap + 1, 1, 128), FLOAT32),
        hub_recv=per_far(dma, (crowd,)),
        hub_sum_recv=per_far(dma, (crowd,)),
        hub_out=per_far(pltpu.VMEM, (blocks,) + query_block, BFLOAT),
        hub_sums_out=per_far(pltpu.VMEM, (blocks, 1, 128), FLOAT32),
        attended=per_head(pltpu.VMEM, (tp, rows, XHEAD), BFLOAT),
        att_send=sems(tp),
        att_recv=sems(tp),
        kept_keys=per_head(pltpu.VMEM, store.shape[:2] + (XHEAD,), BFLOAT),
        kept_values=per_head(pltpu.VMEM, store.shape[:2] + (XHEAD,), BFLOAT),
        m_query=pltpu.VMEM((rows, mix_width), BFLOAT),
        m_key=pltpu.VMEM((rows, mix_width), BFLOAT),
        m_value=pltpu.VMEM((rows, mix_width), BFLOAT),
        m_fade=pltpu.VMEM((rows, mix_width), FLOAT32),
        m_gate=pltpu.VMEM((rows, mix_width), FLOAT32),
        state=pltpu.VMEM((mix_width // size.mix_heads, mix_width), FLOAT32),
        mixed=pltpu.VMEM((tp, rows, mix_width), BFLOAT),
        mix_send=dma((tp,)),
        mix_recv=dma((tp,)),
        opened=pltpu.VMEM((rows, out_cols), FLOAT32),
        mix_acc=pltpu.VMEM((rows, out_cols), FLOAT32),
        cross_acc=pltpu.VMEM((rows, out_cols), FLOAT32),
    )
    out_shape = jax.ShapeDtypeStruct((rows, out_cols), BFLOAT)
    given = (passage_ids.T, small, big)
    leaves, tree = jax.tree.flatten((*given, out_shape, scratch))
    flat = jax.tree.leaves(given)
    spaces = [pltpu.SMEM] + [pl.ANY] * (len(small) + len(big))
    return pl.pallas_call(
        functools.partial(layer_kernel, size, tree),
        in_specs=[pl.BlockSpec(memory_space=space) for space in spaces],
        out_specs=pl.BlockSpec(memory_space=pltpu.VMEM),
        out_shape=out_shape,
        scratch_shapes=leaves[len(flat) + 1 :],
        compiler_params=pltpu.CompilerParams(
            collective_id=0, has_side_effects=True, vmem_limit_bytes=67043328
        ),
    )(*flat)


def solution(mesh):
    placed = (
        P(ST, None),
        P(None, TP),
        P(None, TP),
        P(None, TP),
        P(),
        P(None, TP),
        P(TP),
        P(ST, TP),
        P(),
        P(None, TP),
        P(TP),
        P(None, TP),
        P(None, TP),
        P(TP),
        P(None, TP),
        P(None, TP),
        P(None, TP),
        P(),
        P(None, TP),
        P(ST, None, None),
        P(ST, None),
    )
    return jax.shard_map(layer, mesh=mesh, in_specs=placed, out_specs=P(ST, TP), check_vma=False)
```

```python
import contextlib
import functools

import jax
import jax.numpy as jnp
from jax import lax
from jax.experimental import pallas as pl
from jax.experimental.pallas import tpu as pltpu
from jax.sharding import PartitionSpec as P

XHEAD = 256
QBLOCK = 64
MBLOCK = 64

FLOAT32 = jnp.float32
BFLOAT = jnp.bfloat16
MESH = pl.DeviceIdType.MESH
scope = contextlib.nullcontext
ST, TP = "st", "tp"


def split(values):
    high = values.astype(BFLOAT)
    return high, (values - high.astype(FLOAT32)).astype(BFLOAT)


def raw_dot(left, right, dims=((1,), (0,))):
    return lax.dot_general(left, right, (dims, ((), ())), preferred_element_type=FLOAT32)


def fine_dot(left, right, dims=((1,), (0,))):
    left = left[0] if isinstance(left, tuple) else left.astype(BFLOAT)
    right = right[0] if isinstance(right, tuple) else right.astype(BFLOAT)
    return raw_dot(left, right, dims)


def exact_dot(values, ones):
    return raw_dot(values.astype(BFLOAT), ones)


def iota(shape, dim):
    return lax.broadcasted_iota(jnp.int32, shape, dim)


def each(fn, *lists):
    return [fn(*items) for items in zip(*lists)]


def recur_step(heads, blocks, base, refs, gain, state_ref, out_ref):
    query_ref, key_ref, value_ref, fade_ref, gate_ref = refs
    width = query_ref.shape[1]
    size = width // heads
    rows = heads * MBLOCK
    row_head = (iota((rows, width), 0) // MBLOCK) == (iota((rows, width), 1) // size)
    state_head = (iota((width, width), 0) // size) == (iota((width, width), 1) // size)
    ones_head = jnp.where(state_head, 1.0, 0.0).astype(BFLOAT)
    row_pos = iota((rows, rows), 0) % MBLOCK
    col_pos = iota((rows, rows), 1) % MBLOCK
    strict = col_pos < row_pos
    upto = col_pos <= row_pos
    lower = jnp.where(
        iota((MBLOCK, MBLOCK), 1) <= iota((MBLOCK, MBLOCK), 0), 1.0, 0.0
    ).astype(BFLOAT)

    def expand(values):
        return jnp.where(row_head, jnp.concatenate([values] * heads, axis=0), 0.0)

    def compact(values):
        return jnp.concatenate(
            [values[:, head * size : (head + 1) * size] for head in range(heads)], axis=0
        )

    def natural(values):
        return jnp.concatenate(
            [values[head * MBLOCK : (head + 1) * MBLOCK] for head in range(heads)], axis=1
        )

    def span(block):
        return pl.ds(pl.multiple_of(base + block * MBLOCK, MBLOCK), MBLOCK)

    def load(ref):
        return [ref[span(b), :].astype(FLOAT32) for b in range(blocks)]

    def running_sum(fade):
        high, low = split(fade)
        rest = (fade - high.astype(FLOAT32) - low.astype(FLOAT32)).astype(BFLOAT)
        return raw_dot(lower, high) + (raw_dot(lower, low) + raw_dot(lower, rest))

    query, key, value = load(query_ref), load(key_ref), load(value_ref)
    fade, gate = load(fade_ref), load(gate_ref)
    cumul = each(running_sum, fade)
    unit = each(lambda k: k * lax.rsqrt(exact_dot(k * k, ones_head) + 1e-06), key)
    rate = each(lambda u, g: u * g, unit, gate)
    minus_scaled = each(lambda u, c, f: -u * jnp.exp(c - f), unit, cumul, fade)
    query_scaled = each(lambda q, c: q * jnp.exp(c), query, cumul)
    inverse = each(lambda c: jnp.exp(-c), cumul)
    fade_out = each(lambda c: jnp.exp(c[MBLOCK - 1 :, :] - c), cumul)
    block_fade = each(lambda c: jnp.exp(c[MBLOCK - 1 :, :]), cumul)
    left = each(
        lambda m, q: split(jnp.concatenate([expand(m), expand(q)], axis=0)),
        minus_scaled,
        query_scaled,
    )
    right = each(
        lambda k, r, i: split(jnp.concatenate([expand(k * i), expand(r * i)], axis=0)),
        key,
        rate,
        inverse,
    )
    pairs = each(lambda a, b: fine_dot(a, b, ((1,), (1,))), left, right)
    key_mats = each(
        lambda p: jnp.concatenate(
            [jnp.where(strict, p[:rows, :rows], 0.0), jnp.where(upto, p[rows:, :rows], 0.0)], axis=0
        ),
        pairs,
    )
    rate_pull = each(lambda p: split(jnp.where(strict, p[:rows, rows:], 0.0)), pairs)
    rate_read = each(lambda p: split(jnp.where(upto, p[rows:, rows:], 0.0)), pairs)
    value_rows = each(lambda v: compact(v).astype(BFLOAT), value)

    def key_values(mats, vals):
        return raw_dot(mats.astype(BFLOAT), vals)

    from_values = each(key_values, key_mats, value_rows)
    solved = each(
        lambda m, kv: jnp.concatenate([compact(m), kv[:rows]], axis=1), minus_scaled, from_values
    )
    power = rate_pull
    levels = (MBLOCK - 1).bit_length()
    for level in range(levels):
        solved = each(lambda s, p: s + fine_dot(p, s), solved, power)
        if level < levels - 1:
            power = each(lambda p: split(fine_dot(p, p)), power)
    solved_halves = each(split, solved)
    reads = each(
        lambda q, kv, r, s: jnp.concatenate([compact(q), kv[rows:]], axis=1) + fine_dot(r, s),
        query_scaled,
        from_values,
        rate_read,
        solved_halves,
    )
    moved = each(
        lambda s, r, f: fine_dot(s, expand(r * f), ((0,), (0,))), solved_halves, rate, fade_out
    )

    def key_update(vals, k, f):
        return raw_dot(vals, expand(k * f).astype(BFLOAT), ((0,), (0,)))

    added = each(key_update, value_rows, key, fade_out)
    carry = each(
        lambda m: split(jnp.where(state_head, jnp.concatenate([m[:size]] * heads, axis=0), 0.0)),
        moved,
    )
    added = each(lambda a, m: a + m[size:], added, moved)
    read_state = each(lambda r: split(natural(r[:, :size])), reads)
    read_fixed = each(lambda r: natural(r[:, size:]), reads)
    state = state_ref[...]
    head_out = []
    for block in range(blocks):
        spread_state = jnp.where(state_head, jnp.concatenate([state] * heads, axis=0), 0.0)
        head_out.append(
            read_fixed[block] + fine_dot(read_state[block], spread_state, ((1,), (1,)))
        )
        state = state * block_fade[block] + fine_dot(state, carry[block]) + added[block]
    state_ref[...] = state
    for block in range(blocks):
        mean = exact_dot(head_out[block], ones_head) * (1.0 / size)
        centred = head_out[block] - mean
        variance = exact_dot(centred * centred, ones_head) * (1.0 / size)
        normed = centred * lax.rsqrt(variance + 0.00064) * gain
        out_ref[0, span(block), :] = normed.astype(BFLOAT)


class Names(dict):
    __getattr__ = dict.__getitem__


def remote(src, dst, send, recv, **peer):
    return pltpu.make_async_remote_copy(
        src_ref=src,
        dst_ref=dst,
        send_sem=send,
        recv_sem=recv,
        device_id=peer,
        device_id_type=MESH,
    )


def when(valid, action):
    if valid is True:
        action()
    else:
        pl.when(valid)(action)


def layer_kernel(size, tree, *refs):
    ids, given, big, out, keep = jax.tree.unflatten(tree, refs)
    keep = Names(keep)
    small = Names(keep.small)
    n, tp, depth, wide = size.owners, size.tp, size.depth, size.wide
    lines = tp // 2
    cap, heads, per_block = size.capacity, size.cross_heads, size.per_block
    me = lax.axis_index(ST)
    mine = lax.axis_index(TP)
    level, column = me // wide, me % wide
    half = depth // 2
    upper = level // half
    base = upper * half
    hub = half - 1 + upper
    off_hub = upper * (level - hub) + (1 - upper) * (hub - level)
    hubbed = range(0)

    def seating(head):
        if head in hubbed:
            return base * wide, half * wide
        return 0, n

    line, core = mine // 2, mine % 2
    sibling = line * 2 + 1 - core

    loads = [
        pltpu.make_async_copy(src, dst, keep.load_sem.at[i])
        for i, (src, dst) in enumerate(zip(big, keep.big))
    ]
    (
        load_tokens,
        load_query,
        load_store,
        load_key,
        load_value,
        load_mix_query,
        load_mix_key,
        load_mix_value,
        load_decay,
        load_rate,
        load_gate,
        load_mix_out,
        load_cross,
    ) = loads
    (
        tokens,
        cross_query,
        store,
        passage_key,
        passage_value,
        mix_query,
        mix_key,
        mix_value,
        decay_lower,
        rate_lower,
        gate_down,
        mix_out,
        cross_out,
    ) = keep.big
    little = {
        name: pltpu.make_async_copy(given[name], small[name], keep.small_sem.at[i])
        for i, name in enumerate(given)
    }
    load_tokens.start()
    load_query.start()
    for copy in little.values():
        copy.start()

    barrier = pltpu.get_barrier_semaphore()

    @pl.loop(1, n)
    def _(d):
        pl.semaphore_signal(barrier, inc=1, device_id={ST: (me + d) % n}, device_id_type=MESH)

    for k in range(1, lines):
        peer = ((line + k) % lines) * 2 + core
        pl.semaphore_signal(barrier, inc=1, device_id={TP: peer}, device_id_type=MESH)
    pl.semaphore_signal(barrier, inc=1, device_id={TP: sibling}, device_id_type=MESH)

    slots = size.blocks * per_block
    down_slot = iota((slots, 128), 0)
    lane = iota((slots, 128), 1)
    by_lane = jnp.zeros((slots, 128), jnp.int32)
    by_slot = jnp.zeros((slots, 128), jnp.int32)
    for j in range(slots):
        ident = ids[j % per_block, j // per_block]
        by_lane = jnp.where(lane == j, ident, by_lane)
        by_slot = jnp.where(down_slot == j, ident, by_slot)
    owner_lane, owner_slot = by_lane // size.pass_dev, by_slot // size.pass_dev
    same = owner_lane == owner_slot
    valid = lane < slots

    def count(flags, axis):
        total = jnp.sum(jnp.where(flags & valid, 1, 0), axis=axis, keepdims=True)
        return jnp.minimum(total, cap - 1)

    rank_lane = count(same & (down_slot > lane), 0)
    rank_slot = count(same & (lane > down_slot), 1)
    power = jnp.ones((slots, 1), jnp.int32)
    for s in range(1, cap):
        power = jnp.where(rank_slot == s, 64**s, power)
    mine_too = owner_slot == lane - 64
    code = jnp.sum(jnp.where(mine_too, (down_slot + 1) * power, 0), axis=0, keepdims=True)
    table = jnp.where(lane[:1] < 64, by_lane[:1] * 8 + rank_lane, code)
    keep.names_out[...] = table
    keep.names_in[me] = table

    def name_copy(d):
        return remote(
            keep.names_out,
            keep.names_in.at[me],
            keep.name_send,
            keep.name_recv,
            st=(me + d) % n,
        )

    own_names = pltpu.make_async_copy(keep.names_out, keep.own, keep.own_sem)
    own_names.start()

    above = [(k, level - k >= 0, level - k) for k in range(1, depth)]
    below = [(depth - 1 + k, level + k < depth, level + k) for k in range(1, depth)]
    origins = [(0, True, level)] + above + below

    def dense_copy(head, rel, dst, target):
        return remote(
            keep.dense[head][rel],
            keep.dense[head][dst],
            keep.dense_send[head].at[dst],
            keep.dense_recv[head].at[dst],
            st=target,
        )

    def forwards(head, rel):
        moves = []
        if rel < depth - 1:
            copy = dense_copy(head, rel, rel + 1, (me + wide) % n)
            held = level < depth - 1
            moves.append(((level - rel >= 0) & held if rel else held, copy))
        if rel == 0 or depth - 1 < rel < 2 * depth - 2:
            far = rel - depth + 1 if rel else 0
            copy = dense_copy(head, rel, depth + far, (me + n - wide) % n)
            held = level > 0
            moves.append(((level + far < depth) & held if rel else held, copy))
        return moves

    def side_copy(head, rel, turn):
        slot = rel * wide + turn
        return remote(
            keep.side_out[head].at[slot],
            keep.side_in[head].at[slot],
            keep.side_send[head].at[rel * (wide - 1) + turn - 1],
            keep.side_recv[head].at[rel * (wide - 1) + turn - 1],
            st=level * wide + (column + turn) % wide,
        )

    def digit(code, s):
        return jnp.clip((code // 64**s) % 64 - 1, 0, slots - 1)

    def spread_queries(head, rel, row, where):
        for _, copy in forwards(head, rel):
            pl.when(_)(copy.start)
        for turn in range(1, wide):
            target = where * 0 + level * wide + (column + turn) % wide
            code = row(64 + target)
            for s in range(cap):
                keep.side_out[head][rel * wide + turn, s] = keep.dense[head][rel][
                    digit(code, s) // per_block
                ]
            side_copy(head, rel, turn).start()

    def from_served(source):
        return lambda index: keep.served[source, 0, index]

    for copy in little.values():
        copy.wait()
    load_tokens.wait()
    load_query.wait()
    for copy in loads[2:]:
        copy.start()

    for head in range(heads):
        with scope("q"):
            cols = pl.ds(head * XHEAD, XHEAD)
            dots = raw_dot(tokens[...], cross_query[:, cols])
            mean = jnp.mean(dots * dots, axis=-1, keepdims=True)
            queries = (dots * lax.rsqrt(mean + 1e-06) * small.score_gain[:, cols]).astype(BFLOAT)
            keep.dense[head][0][...] = queries.reshape(keep.dense[head][0].shape)
            if head == 0:
                own_names.wait()
                pl.semaphore_wait(barrier, n - 1 + lines)

                @pl.loop(1, n)
                def _(d):
                    name_copy(d).start()

            if head == 0 or not 0:
                spread_queries(head, 0, lambda index: keep.own[0, index], level)

    with scope("kv"):
        load_store.wait()
        load_key.wait()
        load_value.wait()
        length = size.passage_len
        group = 4 if size.pass_dev % 4 == 0 else 1
        chunk = group * length
        for head in range(heads):
            cols = pl.ds(head * XHEAD, XHEAD)

            @pl.loop(0, size.pass_dev // group)
            def _(i):
                rows = pl.ds(pl.multiple_of(i * chunk, chunk), chunk)
                part = pl.ds(i * group, group)
                shape = (group, length, XHEAD)
                dots = raw_dot(store[rows, :], passage_key[:, cols])
                mean = jnp.mean(dots * dots, axis=-1, keepdims=True)
                kept = (dots * lax.rsqrt(mean + 1e-06)).astype(BFLOAT)
                keep.kept_keys[head][part] = kept.reshape(shape)
                dots = raw_dot(store[rows, :], passage_value[:, cols])
                keep.kept_values[head][part] = dots.astype(BFLOAT).reshape(shape)

    with scope("names"):

        rest = keep.names_in.at[pl.ds(0, n - 1)]
        remote(rest, rest, keep.name_send, keep.name_recv, st=me).wait_recv()
        served = pltpu.make_async_copy(keep.names_in, keep.served, keep.served_sem)
        served.start()
        served.wait()

    ones = jnp.ones((8, length), BFLOAT)

    def result_copies(head, source, target, parts, sums, marks):
        seat = me - seating(head)[0]
        span = pl.ds(seat * cap, cap)
        recv, recv_sums = marks
        return (
            remote(
                keep.parts_out[head].at[source],
                parts.at[span],
                keep.part_send[head],
                recv,
                st=target,
            ),
            remote(
                keep.sums_out[head].at[source],
                sums.at[span],
                keep.sum_send[head],
                recv_sums,
                st=target,
            ),
        )

    def send_direct(head, source):
        marks = keep.part_recv[head], keep.sum_recv[head]
        for copy in result_copies(head, source, source, keep.parts[head], keep.sums[head], marks):
            copy.start()

    def send_to_hub(head, source, far):
        target = hub * wide + source % wide
        parts, sums = keep.hub_parts[head][far - 1], keep.hub_sums[head][far - 1]
        marks = keep.hub_recv[head][far - 1], keep.hub_sum_recv[head][far - 1]
        for copy in result_copies(head, source, target, parts, sums, marks):
            copy.start()

    def keep_at_hub(head, source, far):
        span = pl.ds((me - seating(head)[0]) * cap, cap)
        keep.hub_parts[head][far - 1][span] = keep.parts_out[head][source]
        keep.hub_sums[head][far - 1][span] = keep.sums_out[head][source]

    def attend(head, rel, turn, floor):
        source = floor * wide + (column + wide - turn) % wide
        local = rel == 0 and turn == 0
        row = from_served(source)
        code = row(64 + me)
        for s in range(cap):
            slot = digit(code, s)
            passage = lax.div(row(slot), 8) % size.pass_dev
            kept, vals = keep.kept_keys[head][passage], keep.kept_values[head][passage]
            if turn:
                asked = keep.side_in[head][rel * wide + turn, s]
            else:
                asked = keep.dense[head][rel][slot // per_block]
            scores = raw_dot(asked, kept, ((1,), (1,)))
            expon = jnp.exp(scores * XHEAD ** (-0.5)).astype(BFLOAT)
            result = raw_dot(expon, vals).astype(BFLOAT)
            total = raw_dot(ones, expon, ((1,), (1,)))[:1]
            total = jnp.concatenate([total, jnp.zeros_like(total)], axis=1)
            if local:
                seat = me - seating(head)[0]
                keep.parts[head][seat * cap + s] = result
                keep.sums[head][seat * cap + s] = total
            else:
                keep.parts_out[head][source, s] = result
                keep.sums_out[head][source, s] = total
        if not local and (rel == 0 or head not in hubbed):
            send_direct(head, source)
        elif rel:
            k = rel if rel < depth else rel - depth + 1
            away = floor // half != upper
            if k < half:
                pl.when(jnp.logical_not(away))(functools.partial(send_direct, head, source))
            for step in range(half):
                far = k - step
                if 1 <= far <= half:
                    send = send_to_hub if step or turn else keep_at_hub
                    pl.when(away & (off_hub == step))(functools.partial(send, head, source, far))

    def pass_on(head, k):
        for rel, valid, floor in (origins[k], origins[depth - 1 + k]):

            def arrive(rel=rel, floor=floor):
                dense_copy(head, rel, rel, me).wait_recv()
                spread_queries(head, rel, from_served(floor * wide + column), floor)

            pl.when(valid)(arrive)

    def from_side(head, k, among):
        for rel, valid, floor in (origins[k], origins[depth - 1 + k]) if k else origins[:1]:

            def arrive(rel=rel, floor=floor):
                attend(head, rel, 0, floor)
                for turn in range(1, wide):
                    side_copy(head, rel, turn).wait_recv()
                    attend(head, rel, turn, floor)

            pl.when(among if valid is True else valid & among)(arrive)

    def mixer_inputs():
        for copy in loads[5:10]:
            copy.wait()
        for weight, target in (
            (mix_query, keep.m_query),
            (mix_key, keep.m_key),
            (mix_value, keep.m_value),
        ):
            target[...] = raw_dot(tokens[...], weight[...]).astype(BFLOAT)
        low = jnp.tanh(raw_dot(tokens[...], decay_lower[...], ((1,), (1,)))).astype(BFLOAT)
        pre = small.decay_base[...] + raw_dot(low, small.decay_upper_map[...])
        lanes = iota((size.mix_heads, pre.shape[1]), 1) // (pre.shape[1] // size.mix_heads)
        chosen = iota(lanes.shape, 0) == lanes
        chosen = jnp.where(chosen, 1.0, 0.0).astype(BFLOAT)
        shift = small.decay_shift[...]
        high, middle = split(shift)
        rest = (shift - high.astype(FLOAT32) - middle.astype(FLOAT32)).astype(BFLOAT)
        first = ((0,), (0,))
        pre = pre + (
            raw_dot(high, chosen, first)
            + (raw_dot(middle, chosen, first) + raw_dot(rest, chosen, first))
        )
        keep.m_fade[...] = jax.nn.sigmoid(pre) * (-(2.718281828459045**-0.5))
        low = raw_dot(tokens[...], rate_lower[...], ((1,), (1,))).astype(BFLOAT)
        keep.m_gate[...] = jax.nn.sigmoid(raw_dot(low, small.rate_upper_map[...]))

    blocks = 2 if size.tokens % (2 * MBLOCK) == 0 else 1
    steps = size.tokens // (blocks * MBLOCK)

    def recur(first, last):
        @pl.loop(first, last)
        def _(i):
            recur_step(
                size.mix_heads,
                blocks,
                i * (blocks * MBLOCK),
                (keep.m_query, keep.m_key, keep.m_value, keep.m_fade, keep.m_gate),
                small.norm_gain[...],
                keep.state,
                keep.mixed,
            )

    def tp_copy(buf, send, recv, slot_from, slot_to, peer):
        return remote(
            buf.at[slot_from], buf.at[slot_to], send.at[slot_to], recv.at[slot_to], tp=peer
        )

    def tp_first(buf, send, recv):
        copies = [tp_copy(buf, send, recv, 0, 1, sibling)]
        for k in range(1, lines):
            peer = ((line + k) % lines) * 2 + core
            copies.append(tp_copy(buf, send, recv, 0, 2 * k, peer))
        return copies

    def tp_second(buf, send, recv):
        return [tp_copy(buf, send, recv, 2 * k, 2 * k + 1, sibling) for k in range(1, lines)]

    def origin(slot):
        k, flip = slot // 2, slot % 2
        return ((line + lines - k) % lines) * 2 + (1 - core if flip else core)

    def relay(first, second):
        for copy, forward in zip(first[1:], second):
            copy.wait_recv()
            forward.start()

    def products(buf, weights, stride, offset, acc, fresh):
        width = buf.shape[2]
        total = None if fresh else acc[...]
        for slot in range(tp):
            start = pl.multiple_of(origin(slot) * stride + offset, 128)
            term = raw_dot(buf[slot], weights[pl.ds(start, width), :])
            total = term if total is None else total + term
        acc[...] = total

    def gates():
        load_gate.wait()
        low = raw_dot(tokens[...], gate_down[...]).astype(BFLOAT)
        keep.opened[...] = jax.nn.sigmoid(raw_dot(low, small.gate_up[...]))

    diagonal = iota((QBLOCK, QBLOCK), 0) == iota((QBLOCK, QBLOCK), 1)

    def await_crowd(head, parts, sums, marks):
        low, crowd = seating(head)
        for full, sem in zip((parts, sums), marks):
            rest = full.at[pl.ds(0, (crowd - 1) * cap)]
            remote(rest, rest, sem, sem, st=me).wait_recv()

    def gather(head, entry_of, parts, sums, b):
        low, crowd = seating(head)
        total = jnp.zeros((QBLOCK, XHEAD), FLOAT32)
        row = jnp.zeros((1, 128), FLOAT32)
        for p in range(per_block):
            entry = entry_of(b * per_block + p)
            owner = lax.div(lax.div(entry, 8), size.pass_dev) - low
            inside = (owner >= 0) & (owner < crowd)
            index = jnp.where(inside, owner * cap + lax.rem(entry, 8), crowd * cap)
            total = total + parts[index].astype(FLOAT32)
            row = row + sums[index]
        return total, row

    def hub_copies(head, far):
        target = (hub + far - 2 * far * upper) * wide + column
        return (
            remote(
                keep.hub_out[head][far - 1],
                keep.far_parts[head],
                keep.hub_send[head].at[far - 1],
                keep.far_recv[head].at[0],
                st=target,
            ),
            remote(
                keep.hub_sums_out[head][far - 1],
                keep.far_sums[head],
                keep.hub_sum_send[head].at[far - 1],
                keep.far_recv[head].at[1],
                st=target,
            ),
        )

    def serve_hub(head, far):
        parts, sums = keep.hub_parts[head][far - 1], keep.hub_sums[head][far - 1]
        source = (hub + far - 2 * far * upper) * wide + column

        @pl.when(level == hub)
        def _():
            marks = keep.hub_recv[head][far - 1], keep.hub_sum_recv[head][far - 1]
            await_crowd(head, parts, sums, marks)

            @pl.loop(0, size.blocks)
            def _(b):
                total, row = gather(head, from_served(source), parts, sums, b)
                keep.hub_out[head][far - 1][b] = total.astype(BFLOAT)
                keep.hub_sums_out[head][far - 1][b] = row

            for copy in hub_copies(head, far):
                copy.start()

    def combine(head):
        parts, sums = keep.parts[head], keep.sums[head]
        buf = keep.attended[head]
        with scope("wait"):
            await_crowd(head, parts, sums, (keep.part_recv[head], keep.sum_recv[head]))
            if head in hubbed:
                for copy in hub_copies(head, 1):
                    copy.wait_recv()
        with scope("comb"):

            @pl.loop(0, size.blocks)
            def _(b):
                total, row = gather(head, lambda index: keep.own[0, index], parts, sums, b)
                if head in hubbed:
                    total = total + keep.far_parts[head][b].astype(FLOAT32)
                    row = row + keep.far_sums[head][b]
                inverse = 1.0 / row[:, :QBLOCK]
                column = jnp.sum(jnp.where(diagonal, inverse, 0.0), axis=1, keepdims=True)
                rows = pl.ds(pl.multiple_of(b * QBLOCK, QBLOCK), QBLOCK)
                buf[0, rows, :] = (total * column).astype(BFLOAT)

    every = []

    def tp_start(buf, send, recv):
        first, second = tp_first(buf, send, recv), tp_second(buf, send, recv)
        for copy in first:
            copy.start()
        every.append(first + second)
        return first, second

    def tp_finish(first, second):
        first[0].wait_recv()
        for copy in second:
            copy.wait_recv()

    def tp_attended(head):
        return tp_start(keep.attended[head], keep.att_send[head], keep.att_recv[head])

    keep.state[...] = jnp.zeros_like(keep.state)
    for head in hubbed:
        none = pl.ds(half * wide * cap, 1)
        for parts in (keep.parts[head], *keep.hub_parts[head]):
            parts[none] = jnp.zeros((1, QBLOCK, XHEAD), BFLOAT)
        for sums in (keep.sums[head], *keep.hub_sums[head]):
            sums[none] = jnp.zeros((1, 1, 128), FLOAT32)
    last = heads - 1
    hubs = []

    moves = [(k, head) for k in range(1, depth) for head in range(heads)]
    moves.sort(key=lambda move: move[0] + 0.5 * move[1])
    edge = (level == 0) | (level == depth - 1)
    queues = [
        (edge, [(head, 0) for head in range(heads)], [1,2,2,2,1,0]),
        (jnp.logical_not(edge), [(head, 0) for head in range(heads)], [9,9,9,2,0]),
    ]

    done = 0

    def catch_up(lag=None):
        with scope("side"):
            for among, waiting, lags in queues:
                keep_back = lags[0] if lag is None else lag
                if len(lags) > 1:
                    lags.pop(0)
                if len(waiting) > keep_back:
                    waiting.sort()
                while len(waiting) > keep_back:
                    from_side(*waiting.pop(0), among)

    for k, head in moves:
        if (k, head) not in moves[:2] and done < steps:
            with scope("rec"):
                recur(done, done + 1)
            done += 1
        if (k, head) == moves[-1]:
            if done < steps:
                with scope("rec"):
                    recur(done, steps)
            with scope("mixx"):
                mixer_moves = tp_start(keep.mixed, keep.mix_send, keep.mix_recv)
                gates()
        with scope("pass"):
            pass_on(head, k)
        for _, waiting, _ in queues:
            waiting.append((head, k))
        if k >= half and head in hubbed:
            hubs.append((head, k - half + 1))
        catch_up()
        if (k, head) == moves[0]:
            for other in range(1, heads if 0 else 1):
                spread_queries(other, 0, lambda index: keep.own[0, index], level)
            with scope("mixin"):
                mixer_inputs()
    catch_up(0)
    with scope("relay"):
        relay(*mixer_moves)
    with scope("hub"):
        for job in hubs:
            serve_hub(*job)
    pending = []
    for head in range(last):
        combine(head)
        pending.append(tp_attended(head))
    with scope("mix"):
        load_mix_out.wait()
        load_cross.wait()
        tp_finish(*mixer_moves)
        products(keep.mixed, mix_out, keep.mixed.shape[2], 0, keep.mix_acc, True)
    combine(last)
    pending.append(tp_attended(last))
    with scope("relay"):
        for copies in pending[:last]:
            relay(*copies)
    def settle():
        rest = keep.names_in.at[pl.ds(0, n - 1)]
        remote(rest, rest, keep.name_send, keep.name_recv, st=me).wait_send()
        for head in range(heads):
            for full, sem in ((keep.parts_out, keep.part_send), (keep.sums_out, keep.sum_send)):
                rest = full[head].at[pl.ds(0, n - 1)]
                remote(rest, rest, sem[head], sem[head], st=me).wait_send()

        @pl.when(level == hub)
        def _():
            for head in hubbed:
                for far in range(1, half + 1):
                    for copy in hub_copies(head, far):
                        copy.wait_send()

        for head in range(heads):
            for rel, valid, floor in origins:
                for held, copy in forwards(head, rel):
                    pl.when(held)(copy.wait_send)
                for turn in range(1, wide):
                    when(valid, side_copy(head, rel, turn).wait_send)

    for head in range(heads):
        if head == last:
            with scope("settle"):
                settle()
        with scope("tpx"):
            if head == last:
                relay(*pending[head])
            tp_finish(*pending[head])
        with scope("cross"):
            buf = keep.attended[head]
            products(buf, cross_out, heads * XHEAD, head * XHEAD, keep.cross_acc, head == 0)

    with scope("out"):
        out[...] = (keep.mix_acc[...] + keep.opened[...] * keep.cross_acc[...]).astype(BFLOAT)

    for copies in every:
        for copy in copies:
            copy.wait_send()


def layer(
    tokens,
    mix_query,
    mix_key,
    mix_value,
    decay_lower_map,
    decay_upper_map,
    decay_base,
    decay_shift,
    rate_lower_map,
    rate_upper_map,
    norm_gain,
    mix_out,
    cross_query,
    score_gain,
    passage_key,
    passage_value,
    cross_out,
    gate_down,
    gate_up,
    store,
    passage_ids,
):
    n, tp = lax.axis_size(ST), lax.axis_size(TP)
    rows, model = tokens.shape
    blocks, per_block = passage_ids.shape
    wide = 1
    while n % (2 * wide) == 0 and (2 * wide) ** 2 <= n:
        wide = 2 * wide
    depth = n // wide
    heads = cross_query.shape[1] // XHEAD
    size = Names(
        owners=n,
        tp=tp,
        wide=wide,
        depth=depth,
        tokens=rows,
        blocks=blocks,
        per_block=per_block,
        pass_dev=store.shape[0],
        passage_len=store.shape[1],
        capacity=max(2, -(-(blocks * per_block) // n)),
        cross_heads=heads,
        mix_heads=decay_shift.shape[1],
    )
    cap = size.capacity
    mix_width = mix_query.shape[1]
    out_cols = mix_out.shape[1]
    relatives = 2 * depth - 1
    small = dict(
        decay_upper_map=decay_upper_map,
        decay_base=decay_base.reshape(1, -1),
        decay_shift=decay_shift.T,
        rate_upper_map=rate_upper_map,
        norm_gain=norm_gain.reshape(1, -1),
        score_gain=score_gain.reshape(1, -1),
        gate_up=gate_up,
    )
    big = (
        tokens,
        cross_query,
        store.reshape(-1, model),
        passage_key,
        passage_value,
        mix_query,
        mix_key,
        mix_value,
        decay_lower_map.T,
        rate_lower_map.T,
        gate_down,
        mix_out,
        cross_out,
    )
    dma = pltpu.SemaphoreType.DMA

    def per_head(make, *shape):
        return [make(*shape) for _ in range(heads)]

    def sems(count):
        return [dma((count,)) for _ in range(heads)]

    def per_far(make, *shape):
        return [[make(*shape) for _ in range(half)] for _ in range(0)]

    query_block = (QBLOCK, XHEAD)
    half = depth // 2
    crowd = half * wide
    crowds = [n] * heads
    scratch = dict(
        big=tuple(pltpu.VMEM(array.shape, array.dtype) for array in big),
        load_sem=dma((len(big),)),
        small={name: pltpu.VMEM(array.shape, array.dtype) for name, array in small.items()},
        small_sem=dma((len(small),)),
        own=pltpu.SMEM((1, 128), jnp.int32),
        own_sem=dma,
        served=pltpu.SMEM((n, 1, 128), jnp.int32),
        served_sem=dma,
        names_out=pltpu.VMEM((1, 128), jnp.int32),
        names_in=pltpu.VMEM((n, 1, 128), jnp.int32),
        name_send=dma,
        name_recv=dma,
        dense=[
            [pltpu.VMEM((blocks,) + query_block, BFLOAT) for _ in range(relatives)]
            for _ in range(heads)
        ],
        dense_send=sems(relatives),
        dense_recv=sems(relatives),
        side_out=per_head(pltpu.VMEM, (relatives * wide, cap) + query_block, BFLOAT),
        side_in=per_head(pltpu.VMEM, (relatives * wide, cap) + query_block, BFLOAT),
        side_send=sems(relatives * (wide - 1)),
        side_recv=sems(relatives * (wide - 1)),
        parts_out=per_head(pltpu.VMEM, (n, cap) + query_block, BFLOAT),
        parts=[pltpu.VMEM((c * cap + 1,) + query_block, BFLOAT) for c in crowds],
        part_send=[dma] * heads,
        part_recv=[dma] * heads,
        sums_out=per_head(pltpu.VMEM, (n, cap, 1, 128), FLOAT32),
        sums=[pltpu.VMEM((c * cap + 1, 1, 128), FLOAT32) for c in crowds],
        sum_send=[dma] * heads,
        sum_recv=[dma] * heads,
        hub_parts=per_far(pltpu.VMEM, (crowd * cap + 1,) + query_block, BFLOAT),
        hub_sums=per_far(pltpu.VMEM, (crowd * cap + 1, 1, 128), FLOAT32),
        hub_recv=per_far(dma, (crowd,)),
        hub_sum_recv=per_far(dma, (crowd,)),
        hub_out=per_far(pltpu.VMEM, (blocks,) + query_block, BFLOAT),
        hub_sums_out=per_far(pltpu.VMEM, (blocks, 1, 128), FLOAT32),
        attended=per_head(pltpu.VMEM, (tp, rows, XHEAD), BFLOAT),
        att_send=sems(tp),
        att_recv=sems(tp),
        kept_keys=per_head(pltpu.VMEM, store.shape[:2] + (XHEAD,), BFLOAT),
        kept_values=per_head(pltpu.VMEM, store.shape[:2] + (XHEAD,), BFLOAT),
        m_query=pltpu.VMEM((rows, mix_width), BFLOAT),
        m_key=pltpu.VMEM((rows, mix_width), BFLOAT),
        m_value=pltpu.VMEM((rows, mix_width), BFLOAT),
        m_fade=pltpu.VMEM((rows, mix_width), FLOAT32),
        m_gate=pltpu.VMEM((rows, mix_width), FLOAT32),
        state=pltpu.VMEM((mix_width // size.mix_heads, mix_width), FLOAT32),
        mixed=pltpu.VMEM((tp, rows, mix_width), BFLOAT),
        mix_send=dma((tp,)),
        mix_recv=dma((tp,)),
        opened=pltpu.VMEM((rows, out_cols), FLOAT32),
        mix_acc=pltpu.VMEM((rows, out_cols), FLOAT32),
        cross_acc=pltpu.VMEM((rows, out_cols), FLOAT32),
    )
    out_shape = jax.ShapeDtypeStruct((rows, out_cols), BFLOAT)
    given = (passage_ids.T, small, big)
    leaves, tree = jax.tree.flatten((*given, out_shape, scratch))
    flat = jax.tree.leaves(given)
    spaces = [pltpu.SMEM] + [pl.ANY] * (len(small) + len(big))
    return pl.pallas_call(
        functools.partial(layer_kernel, size, tree),
        in_specs=[pl.BlockSpec(memory_space=space) for space in spaces],
        out_specs=pl.BlockSpec(memory_space=pltpu.VMEM),
        out_shape=out_shape,
        scratch_shapes=leaves[len(flat) + 1 :],
        compiler_params=pltpu.CompilerParams(
            collective_id=0, has_side_effects=True, vmem_limit_bytes=67043328
        ),
    )(*flat)


def solution(mesh):
    placed = (
        P(ST, None),
        P(None, TP),
        P(None, TP),
        P(None, TP),
        P(),
        P(None, TP),
        P(TP),
        P(ST, TP),
        P(),
        P(None, TP),
        P(TP),
        P(None, TP),
        P(None, TP),
        P(TP),
        P(None, TP),
        P(None, TP),
        P(None, TP),
        P(),
        P(None, TP),
        P(ST, None, None),
        P(ST, None),
    )
    return jax.shard_map(layer, mesh=mesh, in_specs=placed, out_specs=P(ST, TP), check_vma=False)
```
